32 devices in a mesh: fs: 8 (over z, y), tp: 4 (over x, core).
Axes of the slice: x: 2, y: 2, z: 4, core: 2. Of those that a mesh axis runs over, the one named last changes fastest.
Arguments:
- layer_input: bfloat16 [16384, 2048], P('fs'), may hold values from -6 to 6
- input_cotangent: bfloat16 [16384, 2048], P('fs', 'tp'), may hold values from -6 to 6
- gate_cotangent: bfloat16 [16384, 2048], P('fs', 'tp'), may hold values from -6 to 6
- input_weight: float32 [2048, 2048], P('fs', 'tp'), may hold values from -0.125 to 0.125
- gate_weight: float32 [2048, 2048], P('fs', 'tp'), may hold values from -0.125 to 0.125
- input_basis: bfloat16 [2048, 256], P('fs'), may hold values from -1.81196113 to 1.81196113
- gate_basis: bfloat16 [2048, 256], P('fs'), may hold values from -1.81196113 to 1.81196113
- input_first: float32 [256, 2048], P('fs', 'tp'), may hold values from -10496 to 10496
- input_second: float32 [256, 2048], P('fs', 'tp'), may hold values from 16384 to 491520
- gate_first: float32 [256, 2048], P('fs', 'tp'), may hold values from -10496 to 10496
- gate_second: float32 [256, 2048], P('fs', 'tp'), may hold values from 16384 to 491520
Outputs:
- input_new: float32 [2048, 2048], P('fs', 'tp')
- gate_new: float32 [2048, 2048], P('fs', 'tp')
- input_step: float32 [2048, 2048], P('fs', 'tp')
- gate_step: float32 [2048, 2048], P('fs', 'tp')
- input_first_new: float32 [256, 2048], P('fs', 'tp')
- input_second_new: float32 [256, 2048], P('fs', 'tp')
- gate_first_new: float32 [256, 2048], P('fs', 'tp')
- gate_second_new: float32 [256, 2048], P('fs', 'tp')
- input_copy: bfloat16 [2048, 2048], P(None, 'tp')
- gate_copy: bfloat16 [2048, 2048], P(None, 'tp')
The draws below stay inside these ranges and needn't reach their ends.
All inputs are finite; a program needn't handle non-finite values.
Results may differ from the reference program's by a relative error of at most 0.0055.
Values may be sent and summed in bfloat16 or wider, within the bound.
A program may use at most 64 MiB of HBM per device.

```python
import math
import jax
import jax.numpy as jnp
from jax import lax

D = 2048
W = 2048
RANK = 256
TOKENS = 16384


def basis_draw(key):
    base_key, rough_key = jax.random.split(key)
    base = jnp.clip(jax.random.normal(base_key, (D, RANK), jnp.float32), -6.0, 6.0)
    spread = math.log(10.0)
    position = jnp.arange(D, dtype=jnp.float32) / max(D - 1, 1)
    rough = jax.random.uniform(rough_key, (D, 1), jnp.float32, -0.3, 0.3)
    scale = jnp.exp(spread * position[:, None] + rough) / math.sqrt(D)
    return (base * scale).astype(jnp.bfloat16)


def moment_draw(key):
    base_key, rough_key = jax.random.split(key)
    base = jnp.clip(jax.random.normal(base_key, (RANK, W), jnp.float32), -6.0, 6.0)
    spread = math.log(10.0)
    position = jnp.arange(W, dtype=jnp.float32) / max(W - 1, 1)
    rough = jax.random.uniform(rough_key, (1, W), jnp.float32, -0.3, 0.3)
    scale = jnp.exp(spread * position[None, :] + rough) * math.sqrt(TOKENS)
    return base * scale


def draw_input_basis(key, part):
    return basis_draw(jax.random.fold_in(key, 11))


def draw_gate_basis(key, part):
    return basis_draw(jax.random.fold_in(key, 12))


def draw_input_first(key, part):
    return moment_draw(jax.random.fold_in(key, 21))


def draw_gate_first(key, part):
    return moment_draw(jax.random.fold_in(key, 22))


def shard_levels(key, dims, cuts, low, largest):
    factor_of, own = 1.0, jax.random.fold_in(key, 6)
    for dim, blocks in cuts:
        heights = jnp.exp(jax.random.uniform(jax.random.fold_in(own, dim), (blocks,), jnp.float32, low / len(cuts), largest / len(cuts)))
        factor_of = factor_of * jnp.repeat(heights, dims[dim] // blocks).reshape([-1 if axis == dim else 1 for axis in range(len(dims))])
    return factor_of


def scatter_about(rng, extent, scale, reach, cuts=(), kind=jnp.bfloat16):
    result = scale * jax.random.normal(rng, extent, jnp.float32)
    if cuts:
        result = result * shard_levels(rng, extent, cuts, -0.22, 0.18)
    return jnp.clip(result, -reach, reach).astype(kind)


def setup_inputs(seed: int = 0) -> dict:
    splits = jax.random.split(jax.random.key(seed), 12)
    layer_input = scatter_about(splits[0], (TOKENS, D), 1.0, 6.0, ((0, 8),))
    input_cotangent = scatter_about(splits[1], (TOKENS, W), 1.0, 6.0, ((0, 8), (1, 4)))
    gate_cotangent = scatter_about(splits[2], (TOKENS, W), 1.0, 6.0, ((0, 8), (1, 4)))
    input_weight = scatter_about(splits[3], (D, W), D ** -0.5, 0.125, ((0, 8), (1, 4)), jnp.float32)
    gate_weight = scatter_about(splits[4], (D, W), D ** -0.5, 0.125, ((0, 8), (1, 4)), jnp.float32)
    input_basis = draw_input_basis(jax.random.fold_in(splits[11], 71), 0)
    gate_basis = draw_gate_basis(jax.random.fold_in(splits[11], 71), 0)
    input_first = draw_input_first(jax.random.fold_in(splits[11], 71), 0)
    input_second = jnp.clip(jnp.exp(math.log(491520.0) - 3.4011974 * jax.random.uniform(splits[8], (RANK, W), jnp.float32) ** shard_levels(splits[8], (RANK, W), ((0, 8), (1, 4)), -0.2, 0.2)), 16384.0, 491520.0)
    gate_first = draw_gate_first(jax.random.fold_in(splits[11], 71), 0)
    gate_second = jnp.clip(jnp.exp(math.log(491520.0) - 3.4011974 * jax.random.uniform(splits[10], (RANK, W), jnp.float32) ** shard_levels(splits[10], (RANK, W), ((0, 8), (1, 4)), -0.2, 0.2)), 16384.0, 491520.0)
    return dict(layer_input=layer_input, input_cotangent=input_cotangent, gate_cotangent=gate_cotangent, input_weight=input_weight, gate_weight=gate_weight, input_basis=input_basis, gate_basis=gate_basis, input_first=input_first, input_second=input_second, gate_first=gate_first, gate_second=gate_second)


first_decay = 0.8
second_decay = 0.95
learn_rate = 0.01

def update_one(layer_input, cotangent, weight, basis, first, second):
    gradient = lax.dot_general(layer_input, cotangent, (((0,), (0,)), ((), ())), preferred_element_type=jnp.float32)
    small = jnp.dot(basis.astype(jnp.float32).T, gradient, precision=lax.Precision.HIGHEST)
    first_new = first_decay * first + (1.0 - first_decay) * small
    second_new = second_decay * second + (1.0 - second_decay) * small * small
    direction = (first_new / (jnp.sqrt(second_new) + 1e-08)).astype(jnp.bfloat16)
    update = jnp.dot(basis, direction, preferred_element_type=jnp.float32)
    spread = jnp.sqrt(jnp.sum(update * update) / (D * W) + 1e-06)
    factor = jnp.minimum(1.0, 1.0 / spread)
    step = factor * update
    fresh = weight - learn_rate * step
    return (fresh, step, first_new, second_new, fresh.astype(jnp.bfloat16))

def reference(layer_input, input_cotangent, gate_cotangent, input_weight, gate_weight, input_basis, gate_basis, input_first, input_second, gate_first, gate_second):
    in_new, in_step, in_first, in_second, in_copy = update_one(layer_input, input_cotangent, input_weight, input_basis, input_first, input_second)
    gt_new, gt_step, gt_first, gt_second, gt_copy = update_one(layer_input, gate_cotangent, gate_weight, gate_basis, gate_first, gate_second)
    return (in_new, gt_new, in_step, gt_step, in_first, in_second, gt_first, gt_second, in_copy, gt_copy)
```

```python
import functools

import jax
import jax.numpy as jnp
from jax import lax
from jax.experimental import pallas as pl
from jax.experimental.pallas import tpu as pltpu
from jax.sharding import PartitionSpec as P

first_decay = 0.8
second_decay = 0.95
learn_rate = 0.01
ANY = pl.BlockSpec(memory_space=pl.ANY)
VMEM = pl.BlockSpec(memory_space=pltpu.VMEM)
MESH = pl.DeviceIdType.MESH
f32, bf16 = jnp.float32, jnp.bfloat16


def moments(small, first, second):
    first_new = first_decay * first + (1.0 - first_decay) * small
    second_new = second_decay * second + (1.0 - second_decay) * small * small
    return first_new, second_new


def remote(src, dst, send, recv, **axis):
    return pltpu.make_async_remote_copy(
        src_ref=src, dst_ref=dst, send_sem=send, recv_sem=recv, device_id=axis, device_id_type=MESH
    )


def exchange(
    n, tp, x_hbm, ci_hbm, cg_hbm, wi_hbm, wg_hbm, bi_hbm, bg_hbm, first, second,
    weights, basis_out, dir_out, small_out, squares_out,
    xs, cs, ball, wf, wb, proj, acc, part, recvp, dirs, dirf, sq,
    xsem, csem, bsem, wsem, osem,
    b_s, b_r, x_s, x_r, c_s, c_r, d_s, d_r, p_s, p_r, g_s, g_r, q_s, q_r,
    r_s, r_r, l_s, l_r, y_s, y_r,
):
    me, t = lax.axis_index("fs"), lax.axis_index("tp")
    tokens, rb, rank2 = xs.shape[1], ball.shape[1], ball.shape[2]
    group = xs.shape[2] // rb
    rank = rank2 // 2
    rr = rank // n
    wc = cs.shape[2]
    quarter = rb // 4
    tile = min(512, tokens)

    def local(src, dst, sem):
        copy = pltpu.make_async_copy(src, dst, sem)
        copy.start()
        return copy

    def peer(k):
        return lax.rem(me + k, n)

    def origin(k):
        return lax.rem(me + n - k, n)

    b_in = [
        local(ref, ball.at[me, :, pl.ds(p * rank, rank)], bsem.at[p])
        for p, ref in enumerate((bi_hbm, bg_hbm))
    ]
    x_in = []
    wide = rb * group
    for k in range(n // group):
        at = pl.multiple_of(origin(k) * rb, rb) if group == 1 else k * wide
        x_in.append(local(x_hbm.at[:, pl.ds(at, wide)], xs.at[k], xsem.at[k]))
    w_in = [local(ref, wf.at[p], wsem.at[p]) for p, ref in enumerate((wi_hbm, wg_hbm))]
    c_in = [local(ref, cs.at[p], csem.at[p]) for p, ref in enumerate((ci_hbm, cg_hbm))]

    barrier = pltpu.get_barrier_semaphore()
    for k in range(1, n):
        pl.semaphore_signal(barrier, inc=1, device_id={"fs": peer(k)}, device_id_type=MESH)
    for k in range(1, tp):
        pl.semaphore_signal(barrier, inc=1, device_id={"tp": lax.rem(t + k, tp)}, device_id_type=MESH)
    pl.semaphore_wait(barrier, n + tp - 2)

    q = lax.rem(t, 4)
    base = t - q
    qx = lax.rem(q + 2, 4)
    qc = q + 1 - 2 * lax.rem(q, 2)
    qd = lax.rem(qc + 2, 4)

    def rows(j, which):
        return ball.at[j, pl.ds(pl.multiple_of(which * quarter, quarter), quarter), :]

    for copy in b_in:
        copy.wait()
    pending = []
    b_copies = {}
    for k in range(1, n):
        b_copies[k] = remote(rows(me, q), rows(me, q), b_s.at[k], b_r.at[k], fs=peer(k))
        b_copies[k].start()
        pending.append(b_copies[k])

    def product(k, j):
        x_in[k].wait()

        def body(i, _):
            at = pl.ds(pl.multiple_of(i * tile, tile), tile)
            right = ball[j] if group == 1 else ball[j:j + group].reshape(wide, rank2)
            term = jnp.dot(xs[k, at, :], right, preferred_element_type=f32)
            if k == 0:
                proj[at, :] = term
            else:
                proj[at, :] += term
            return 0

        lax.fori_loop(0, tokens // tile, body, 0)

    def got(ref, sem):
        pltpu.make_async_copy(ref, ref, sem).wait()

    for k in range(n + 2):
        if 1 <= k < n:
            j = origin(k)
            got(rows(j, q), b_r.at[k])
            for ss, sr, to in ((x_s, x_r, qx), (c_s, c_r, qc)):
                copy = remote(rows(j, q), rows(j, q), ss.at[k], sr.at[k], tp=base + to)
                copy.start()
                pending.append(copy)
        if 1 <= k - 1 < n:
            j = origin(k - 1)
            got(rows(j, qx), x_r.at[k - 1])
            copy = remote(rows(j, qx), rows(j, qx), d_s.at[k - 1], d_r.at[k - 1], tp=base + qc)
            copy.start()
            pending.append(copy)
        if k == 0:
            if group == 1:
                product(0, me)
            for p in range(2):
                w_in[p].wait()
                wb[p] = wf[p].astype(bf16)
        if k >= 3:
            j = origin(k - 2)
            got(rows(j, qc), c_r.at[k - 2])
            got(rows(j, qd), d_r.at[k - 2])
            if group == 1:
                product(k - 2, j)
    if group > 1:
        for k in range(n // group):
            product(k, k * group)

    length = n // 2
    a, b = me // 2, lax.rem(me, 2)
    waits = []

    def guarded(here, copy, start=True):
        if start:
            @pl.when(here)
            def _():
                copy.start()
        waits.append((here, copy))

    def block(chain, side):
        safe = jnp.clip(chain, 0, length - 1)
        return weights.at[safe * 2 + side]

    def send_weights(s):
        for sign, ss, sr in ((1, r_s, r_r), (-1, l_s, l_r)):
            chain = a - sign * (s - 1)
            exists = jnp.logical_and(chain >= 0, chain < length)
            place = block(chain, b)
            src = wb if s == 1 else place
            slot = (s - 1) * 2 + (0 if sign == 1 else 1)
            if s > 1:
                @pl.when(exists)
                def _():
                    got(place, sr.at[s - 1])
            if s < length:
                after = a + sign
                inside = jnp.logical_and(after >= 0, after < length)
                to = jnp.clip(after, 0, length - 1) * 2 + b
                guarded(jnp.logical_and(exists, inside), remote(src, place, ss.at[s], sr.at[s], fs=to))
            if s > 1 or sign == 1:
                guarded(exists, remote(src, place, y_s.at[slot], y_r.at[slot], fs=a * 2 + 1 - b))

    send_weights(1)

    for p in range(2):
        c_in[p].wait()

        def body(i, _):
            at = pl.ds(pl.multiple_of(i * tile, tile), tile)
            term = lax.dot_general(
                proj[at, p * rank:(p + 1) * rank].astype(bf16), cs[p, at, :],
                (((0,), (0,)), ((), ())), preferred_element_type=f32,
            )
            acc[p] += term
            return 0

        acc[p] = jnp.zeros_like(acc[p])
        lax.fori_loop(0, tokens // tile, body, 0)
        for j in range(n):
            part[j, p] = acc[p, j * rr:(j + 1) * rr, :].astype(bf16)
    for k in range(1, n):
        copy = remote(part.at[peer(k)], recvp.at[k], p_s.at[k], p_r.at[k], fs=peer(k))
        copy.start()
        pending.append(copy)
    out_basis = local(ball, basis_out, osem.at[0])
    send_weights(2)
    own = pl.ds(pl.multiple_of(me * rr, rr), rr)
    total = acc[:, own, :]
    for k in range(1, n):
        got(recvp.at[k], p_r.at[k])
        total = total + recvp[k].astype(f32)
    small_out[...] = total
    first_new, second_new = moments(total, first[...], second[...])
    dirs[0] = (first_new / (jnp.sqrt(second_new) + 1e-08)).astype(bf16)
    for k in range(1, n):
        copy = remote(dirs.at[0], dirs.at[k], g_s.at[k], g_r.at[k], fs=peer(k))
        copy.start()
        pending.append(copy)
    for s in range(3, length + 1):
        if s == 3:
            send_weights(s)
    dirf[:, own, :] = dirs[0].astype(f32)
    for k in range(1, n):
        got(dirs.at[k], g_r.at[k])
        dirf[:, pl.ds(pl.multiple_of(origin(k) * rr, rr), rr), :] = dirs[k].astype(f32)
    for p in range(2):
        dir_out[p] = dirf[p].astype(bf16)
        sq[0, p] = jnp.zeros_like(sq[0, p])

        def body(j, _):
            update = jnp.dot(
                ball[j, :, p * rank:(p + 1) * rank], dir_out[p], preferred_element_type=f32
            )
            square = jnp.sum((update * update).reshape(rb // 8, 8, wc), axis=0)
            lanes = square[:, :128]
            for at in range(128, wc, 128):
                lanes = lanes + square[:, at:at + 128]
            sq[0, p] += lanes
            return 0

        lax.fori_loop(0, n, body, 0)
    for k in range(1, tp):
        copy = remote(sq.at[0], sq.at[k], q_s.at[k], q_r.at[k], tp=lax.rem(t + k, tp))
        copy.start()
        pending.append(copy)
    for s in range(4, length + 1):
        send_weights(s)
    summed = sq[0]
    for k in range(1, tp):
        got(sq.at[k], q_r.at[k])
        summed = summed + sq[k]
    squares_out[...] = summed
    out_basis.wait()
    for s in range(1, length + 1):
        for sign in (1, -1):
            if s == 1 and sign == -1:
                continue
            chain = a - sign * (s - 1)
            slot = (s - 1) * 2 + (0 if sign == 1 else 1)

            @pl.when(jnp.logical_and(chain >= 0, chain < length))
            def _():
                got(block(chain, 1 - b), y_r.at[slot])
    for here, copy in waits:
        @pl.when(here)
        def _():
            copy.wait_send()
    for copy in pending:
        copy.wait_send()


def finish(
    wi, wg, all_w, ball, dirs, small, squares, first, second, count_ref,
    new_i, new_g, step_i, step_g, fi, si, fg, sg, copy_i, copy_g,
):
    j = pl.program_id(0)
    me = lax.axis_index("fs")
    rank = dirs.shape[1]

    @pl.when(j == 0)
    def _():
        first_new, second_new = moments(small[...], first[...], second[...])
        fi[...], fg[...] = first_new[0], first_new[1]
        si[...], sg[...] = second_new[0], second_new[1]

    for p, (w, new, step, copy) in enumerate(((wi, new_i, step_i, copy_i), (wg, new_g, step_g, copy_g))):
        mean = jnp.sum(squares[p], keepdims=True) * count_ref[0]
        factor = jnp.minimum(1.0, 1.0 / jnp.sqrt(mean + 1e-06))
        update = jnp.dot(ball[0, :, p * rank:(p + 1) * rank], dirs[p], preferred_element_type=f32)
        scaled = factor * update

        @pl.when(j == me)
        def _():
            step[...] = scaled
            fresh = w[...] - learn_rate * scaled
            new[...] = fresh
            copy[...] = fresh.astype(bf16)

        @pl.when(j != me)
        def _():
            copy[...] = (all_w[0, p].astype(f32) - learn_rate * scaled).astype(bf16)


def shards(n, tp, x, ci, cg, wi, wg, bi, bg, fi, si, fg, sg):
    tokens, width = x.shape
    wc, (rb, rank), rr = ci.shape[1], bi.shape, fi.shape[0]
    length = n // 2
    group = max(1, 128 // rb)
    first, second = jnp.stack([fi, fg]), jnp.stack([si, sg])
    dma = pltpu.SemaphoreType.DMA
    all_w, ball, dirs, small, squares = pl.pallas_call(
        functools.partial(exchange, n, tp),
        out_shape=(
            jax.ShapeDtypeStruct((n, 2, rb, wc), bf16),
            jax.ShapeDtypeStruct((n, rb, 2 * rank), bf16),
            jax.ShapeDtypeStruct((2, rank, wc), bf16),
            jax.ShapeDtypeStruct((2, rr, wc), f32),
            jax.ShapeDtypeStruct((2, 8, 128), f32),
        ),
        in_specs=[ANY] * 7 + [VMEM] * 2,
        out_specs=(ANY, ANY, VMEM, VMEM, VMEM),
        scratch_shapes=[
            pltpu.VMEM((n // group, tokens, rb * group), bf16),
            pltpu.VMEM((2, tokens, wc), bf16),
            pltpu.VMEM((n, rb, 2 * rank), bf16),
            pltpu.VMEM((2, rb, wc), f32),
            pltpu.VMEM((2, rb, wc), bf16),
            pltpu.VMEM((tokens, 2 * rank), f32),
            pltpu.VMEM((2, rank, wc), f32),
            pltpu.VMEM((n, 2, rr, wc), bf16),
            pltpu.VMEM((n, 2, rr, wc), bf16),
            pltpu.VMEM((n, 2, rr, wc), bf16),
            pltpu.VMEM((2, rank, wc), f32),
            pltpu.VMEM((tp, 2, 8, 128), f32),
            dma((n,)), dma((2,)), dma((2,)), dma((2,)), dma((1,)),
        ]
        + [dma((n,))] * 12
        + [dma((tp,))] * 2
        + [dma((length + 1,))] * 4
        + [dma((2 * length,))] * 2,
        compiler_params=pltpu.CompilerParams(
            collective_id=0, has_side_effects=True, vmem_limit_bytes=56 * 1024 * 1024
        ),
        name="exchange",
    )(x, ci, cg, wi, wg, bi, bg, first, second)

    def whole(*shape):
        return pl.BlockSpec(shape, lambda j: (0,) * len(shape))

    count = jnp.full((1,), 1.0 / (width * wc * tp), f32)
    return pl.pallas_call(
        finish,
        grid=(n,),
        out_shape=tuple(jax.ShapeDtypeStruct((rb, wc), f32) for _ in range(4))
        + tuple(jax.ShapeDtypeStruct((rr, wc), f32) for _ in range(4))
        + tuple(jax.ShapeDtypeStruct((width, wc), bf16) for _ in range(2)),
        in_specs=[
            whole(rb, wc), whole(rb, wc),
            pl.BlockSpec((1, 2, rb, wc), lambda j: (j, 0, 0, 0)),
            pl.BlockSpec((1, rb, 2 * rank), lambda j: (j, 0, 0)),
            whole(2, rank, wc), whole(2, rr, wc), whole(2, 8, 128), whole(2, rr, wc), whole(2, rr, wc),
            pl.BlockSpec(memory_space=pltpu.SMEM),
        ],
        out_specs=tuple(whole(rb, wc) for _ in range(4))
        + tuple(whole(rr, wc) for _ in range(4))
        + tuple(pl.BlockSpec((rb, wc), lambda j: (j, 0)) for _ in range(2)),
        compiler_params=pltpu.CompilerParams(vmem_limit_bytes=40 * 1024 * 1024),
        name="finish",
    )(wi, wg, all_w, ball, dirs, small, squares, first, second, count)


def solution(mesh):
    cut, rows = P("fs", "tp"), P("fs", None)
    return jax.shard_map(
        functools.partial(shards, mesh.shape["fs"], mesh.shape["tp"]),
        mesh=mesh,
        in_specs=(rows, cut, cut, cut, cut, rows, rows, cut, cut, cut, cut),
        out_specs=(cut,) * 8 + (P(None, "tp"),) * 2,
        check_vma=False,
    )
```

```python
import functools

import jax
import jax.numpy as jnp
from jax import lax
from jax.experimental import pallas as pl
from jax.experimental.pallas import tpu as pltpu
from jax.sharding import PartitionSpec as P

first_decay = 0.8
second_decay = 0.95
learn_rate = 0.01
ANY = pl.BlockSpec(memory_space=pl.ANY)
VMEM = pl.BlockSpec(memory_space=pltpu.VMEM)
MESH = pl.DeviceIdType.MESH
f32, bf16 = jnp.float32, jnp.bfloat16


def moments(small, first, second):
    first_new = first_decay * first + (1.0 - first_decay) * small
    second_new = second_decay * second + (1.0 - second_decay) * small * small
    return first_new, second_new


def remote(src, dst, send, recv, **axis):
    return pltpu.make_async_remote_copy(
        src_ref=src, dst_ref=dst, send_sem=send, recv_sem=recv, device_id=axis, device_id_type=MESH
    )


def exchange(
    n, tp, x_hbm, ci_hbm, cg_hbm, wi_hbm, wg_hbm, bi_hbm, bg_hbm, fi, si, fg, sg,
    weights, basis_out, dir_out, small_out, squares_out,
    xs, cs, ball, wf, wb, proj, acc, part, recvp, dirs, dirf, sq,
    xsem, csem, bsem, wsem, osem,
    b_s, b_r, x_s, x_r, c_s, c_r, d_s, d_r, p_s, p_r, g_s, g_r, q_s, q_r,
    r_s, r_r, l_s, l_r, y_s, y_r,
):
    me, t = lax.axis_index("fs"), lax.axis_index("tp")
    tokens, rb, rank2 = xs.shape[1], ball.shape[1], ball.shape[2]
    group = xs.shape[2] // rb
    rank = rank2 // 2
    rr = rank // n
    wc = cs.shape[2]
    quarter = rb // 4
    tile = min(512, tokens)

    def local(src, dst, sem):
        copy = pltpu.make_async_copy(src, dst, sem)
        copy.start()
        return copy

    def peer(k):
        return lax.rem(me + k, n)

    def origin(k):
        return lax.rem(me + n - k, n)

    b_in = [
        local(ref, ball.at[me, :, pl.ds(p * rank, rank)], bsem.at[p])
        for p, ref in enumerate((bi_hbm, bg_hbm))
    ]
    x_in = []
    wide = rb * group
    for k in range(n // group):
        at = pl.multiple_of(origin(k) * rb, rb) if group == 1 else k * wide
        x_in.append(local(x_hbm.at[:, pl.ds(at, wide)], xs.at[k], xsem.at[k]))
    w_in = [local(ref, wf.at[p], wsem.at[p]) for p, ref in enumerate((wi_hbm, wg_hbm))]
    c_in = [local(ref, cs.at[p], csem.at[p]) for p, ref in enumerate((ci_hbm, cg_hbm))]

    barrier = pltpu.get_barrier_semaphore()
    for k in range(1, n):
        pl.semaphore_signal(barrier, inc=1, device_id={"fs": peer(k)}, device_id_type=MESH)
    for k in range(1, tp):
        pl.semaphore_signal(barrier, inc=1, device_id={"tp": lax.rem(t + k, tp)}, device_id_type=MESH)
    pl.semaphore_wait(barrier, n + tp - 2)

    q = lax.rem(t, 4)
    base = t - q
    qx = lax.rem(q + 2, 4)
    qc = q + 1 - 2 * lax.rem(q, 2)
    qd = lax.rem(qc + 2, 4)

    def rows(j, which):
        return ball.at[j, pl.ds(pl.multiple_of(which * quarter, quarter), quarter), :]

    for copy in b_in:
        copy.wait()
    pending = []
    b_copies = {}
    for k in range(1, n):
        b_copies[k] = remote(rows(me, q), rows(me, q), b_s.at[k], b_r.at[k], fs=peer(k))
        b_copies[k].start()
        pending.append(b_copies[k])

    def product(k, j):
        x_in[k].wait()

        def body(i, _):
            at = pl.ds(pl.multiple_of(i * tile, tile), tile)
            right = ball[j] if group == 1 else ball[j:j + group].reshape(wide, rank2)
            term = jnp.dot(xs[k, at, :], right, preferred_element_type=f32)
            if k == 0:
                proj[at, :] = term
            else:
                proj[at, :] += term
            return 0

        lax.fori_loop(0, tokens // tile, body, 0)

    def got(ref, sem):
        pltpu.make_async_copy(ref, ref, sem).wait()

    length = n // 2
    a, b = me // 2, lax.rem(me, 2)
    waits = []

    def block(chain, side, p):
        return weights.at[jnp.clip(chain, 0, length - 1) * 2 + side, p]

    def guarded(here, copy):
        @pl.when(here)
        def _():
            copy.start()

        waits.append((here, copy))

    def across(s, sign, p):
        chain = a - sign * (s - 1)
        exists = jnp.logical_and(chain >= 0, chain < length)
        place = block(chain, b, p)
        slot = ((s - 1) * 2 + (0 if sign == 1 else 1)) * 2 + p
        guarded(exists, remote(
            wb.at[p] if s == 1 else place, place, y_s.at[slot], y_r.at[slot], fs=a * 2 + 1 - b))

    def along(s, sign, p):
        chain = a - sign * (s - 1)
        exists = jnp.logical_and(chain >= 0, chain < length)
        place = block(chain, b, p)
        ss, sr = (r_s, r_r) if sign == 1 else (l_s, l_r)
        if s > 1:
            @pl.when(exists)
            def _():
                got(place, sr.at[(s - 1) * 2 + p])
        if s < length:
            after = a + sign
            inside = jnp.logical_and(after >= 0, after < length)
            to = jnp.clip(after, 0, length - 1) * 2 + b
            at = s * 2 + p
            guarded(jnp.logical_and(exists, inside), remote(
                wb.at[p] if s == 1 else place, place, ss.at[at], sr.at[at], fs=to))

    def send_weights(s):
        for p in range(2):
            for sign in (1, -1):
                along(s, sign, p)
                across(s, sign, p)

    for p in range(2):
        w_in[p].wait()
        wb[p] = wf[p].astype(bf16)

    for k in range(n + 2):
        if 1 <= k < n:
            j = origin(k)
            got(rows(j, q), b_r.at[k])
            for ss, sr, to in ((x_s, x_r, qx), (c_s, c_r, qc)):
                copy = remote(rows(j, q), rows(j, q), ss.at[k], sr.at[k], tp=base + to)
                copy.start()
                pending.append(copy)
        if 1 <= k - 1 < n:
            j = origin(k - 1)
            got(rows(j, qx), x_r.at[k - 1])
            copy = remote(rows(j, qx), rows(j, qx), d_s.at[k - 1], d_r.at[k - 1], tp=base + qc)
            copy.start()
            pending.append(copy)
        if k == 0:
            if group == 1:
                product(0, me)
            for p in range(2):
                across(1, 1, p)
        if k == n // 2:
            for p in range(2):
                for sign in (1, -1):
                    along(1, sign, p)
        if k >= 3:
            j = origin(k - 2)
            got(rows(j, qc), c_r.at[k - 2])
            got(rows(j, qd), d_r.at[k - 2])
            if group == 1:
                product(k - 2, j)
    if group > 1:
        for k in range(n // group):
            product(k, k * group)

    for p in range(2):
        c_in[p].wait()

        def body(i, _):
            at = pl.ds(pl.multiple_of(i * tile, tile), tile)
            term = lax.dot_general(
                proj[at, p * rank:(p + 1) * rank].astype(bf16), cs[p, at, :],
                (((0,), (0,)), ((), ())), preferred_element_type=f32,
            )
            acc[p] += term
            return 0

        acc[p] = jnp.zeros_like(acc[p])
        lax.fori_loop(0, tokens // tile, body, 0)
        for j in range(n):
            part[j, p] = acc[p, j * rr:(j + 1) * rr, :].astype(bf16)
    for k in range(1, n):
        copy = remote(part.at[peer(k)], recvp.at[k], p_s.at[k], p_r.at[k], fs=peer(k))
        copy.start()
        pending.append(copy)
    out_basis = local(ball, basis_out, osem.at[0])
    send_weights(2)
    own = pl.ds(pl.multiple_of(me * rr, rr), rr)
    total = acc[:, own, :]
    for k in range(1, n):
        got(recvp.at[k], p_r.at[k])
        total = total + recvp[k].astype(f32)
    small_out[...] = total
    for p, (first, second) in enumerate(((fi, si), (fg, sg))):
        first_new, second_new = moments(total[p], first[...], second[...])
        dirs[0, p] = (first_new / (jnp.sqrt(second_new) + 1e-08)).astype(bf16)
    for k in range(1, n):
        copy = remote(dirs.at[0], dirs.at[k], g_s.at[k], g_r.at[k], fs=peer(k))
        copy.start()
        pending.append(copy)
    for s in range(3, length + 1):
        if s == 3:
            send_weights(s)
    dirf[:, own, :] = dirs[0].astype(f32)
    for k in range(1, n):
        got(dirs.at[k], g_r.at[k])
        dirf[:, pl.ds(pl.multiple_of(origin(k) * rr, rr), rr), :] = dirs[k].astype(f32)
    for p in range(2):
        dir_out[p] = dirf[p].astype(bf16)
        sq[0, p] = jnp.zeros_like(sq[0, p])

        def body(j, _):
            update = jnp.dot(
                ball[j, :, p * rank:(p + 1) * rank], dir_out[p], preferred_element_type=f32
            )
            square = jnp.sum((update * update).reshape(rb // 8, 8, wc), axis=0)
            lanes = square[:, :128]
            for at in range(128, wc, 128):
                lanes = lanes + square[:, at:at + 128]
            sq[0, p] += lanes
            return 0

        lax.fori_loop(0, n, body, 0)
    for k in range(1, tp):
        copy = remote(sq.at[0], sq.at[k], q_s.at[k], q_r.at[k], tp=lax.rem(t + k, tp))
        copy.start()
        pending.append(copy)
    for s in range(4, length + 1):
        send_weights(s)
    summed = sq[0]
    for k in range(1, tp):
        got(sq.at[k], q_r.at[k])
        summed = summed + sq[k]
    squares_out[...] = summed
    out_basis.wait()
    for s in range(1, length + 1):
        for sign in (1, -1):
            if s == 1 and sign == -1:
                continue
            chain = a - sign * (s - 1)
            slot = ((s - 1) * 2 + (0 if sign == 1 else 1)) * 2
            for p in range(2):

                @pl.when(jnp.logical_and(chain >= 0, chain < length))
                def _():
                    got(block(chain, 1 - b, p), y_r.at[slot + p])
    for here, copy in waits:
        @pl.when(here)
        def _():
            copy.wait_send()
    for copy in pending:
        copy.wait_send()


def finish(
    wi, wg, all_w, ball, dirs, small, squares, fi, si, fg, sg, count_ref,
    new_i, new_g, step_i, step_g, fi_new, si_new, fg_new, sg_new, copy_i, copy_g,
):
    j = pl.program_id(0)
    me = lax.axis_index("fs")
    rank = dirs.shape[1]

    @pl.when(j == 0)
    def _():
        fi_new[...], si_new[...] = moments(small[0], fi[...], si[...])
        fg_new[...], sg_new[...] = moments(small[1], fg[...], sg[...])

    for p, (w, new, step, copy) in enumerate(((wi, new_i, step_i, copy_i), (wg, new_g, step_g, copy_g))):
        mean = jnp.sum(squares[p], keepdims=True) * count_ref[0]
        factor = jnp.minimum(1.0, 1.0 / jnp.sqrt(mean + 1e-06))
        update = jnp.dot(ball[0, :, p * rank:(p + 1) * rank], dirs[p], preferred_element_type=f32)
        scaled = factor * update

        @pl.when(j == me)
        def _():
            step[...] = scaled
            fresh = w[...] - learn_rate * scaled
            new[...] = fresh
            copy[...] = fresh.astype(bf16)

        @pl.when(j != me)
        def _():
            copy[...] = (all_w[0, p].astype(f32) - learn_rate * scaled).astype(bf16)


def shards(n, tp, x, ci, cg, wi, wg, bi, bg, fi, si, fg, sg):
    tokens, width = x.shape
    wc, (rb, rank), rr = ci.shape[1], bi.shape, fi.shape[0]
    length = n // 2
    group = max(1, 128 // rb)
    dma = pltpu.SemaphoreType.DMA
    all_w, ball, dirs, small, squares = pl.pallas_call(
        functools.partial(exchange, n, tp),
        out_shape=(
            jax.ShapeDtypeStruct((n, 2, rb, wc), bf16),
            jax.ShapeDtypeStruct((n, rb, 2 * rank), bf16),
            jax.ShapeDtypeStruct((2, rank, wc), bf16),
            jax.ShapeDtypeStruct((2, rr, wc), f32),
            jax.ShapeDtypeStruct((2, 8, 128), f32),
        ),
        in_specs=[ANY] * 7 + [VMEM] * 4,
        out_specs=(ANY, ANY, VMEM, VMEM, VMEM),
        scratch_shapes=[
            pltpu.VMEM((n // group, tokens, rb * group), bf16),
            pltpu.VMEM((2, tokens, wc), bf16),
            pltpu.VMEM((n, rb, 2 * rank), bf16),
            pltpu.VMEM((2, rb, wc), f32),
            pltpu.VMEM((2, rb, wc), bf16),
            pltpu.VMEM((tokens, 2 * rank), f32),
            pltpu.VMEM((2, rank, wc), f32),
            pltpu.VMEM((n, 2, rr, wc), bf16),
            pltpu.VMEM((n, 2, rr, wc), bf16),
            pltpu.VMEM((n, 2, rr, wc), bf16),
            pltpu.VMEM((2, rank, wc), f32),
            pltpu.VMEM((tp, 2, 8, 128), f32),
            dma((n,)), dma((2,)), dma((2,)), dma((2,)), dma((1,)),
        ]
        + [dma((n,))] * 12
        + [dma((tp,))] * 2
        + [dma((2 * length,))] * 4
        + [dma((4 * length,))] * 2,
        compiler_params=pltpu.CompilerParams(
            collective_id=0, has_side_effects=True, vmem_limit_bytes=56 * 1024 * 1024
        ),
        name="exchange",
    )(x, ci, cg, wi, wg, bi, bg, fi, si, fg, sg)

    def whole(*shape):
        return pl.BlockSpec(shape, lambda j: (0,) * len(shape))

    count = jnp.full((1,), 1.0 / (width * wc * tp), f32)
    return pl.pallas_call(
        finish,
        grid=(n,),
        out_shape=tuple(jax.ShapeDtypeStruct((rb, wc), f32) for _ in range(4))
        + tuple(jax.ShapeDtypeStruct((rr, wc), f32) for _ in range(4))
        + tuple(jax.ShapeDtypeStruct((width, wc), bf16) for _ in range(2)),
        in_specs=[
            whole(rb, wc), whole(rb, wc),
            pl.BlockSpec((1, 2, rb, wc), lambda j: (j, 0, 0, 0)),
            pl.BlockSpec((1, rb, 2 * rank), lambda j: (j, 0, 0)),
            whole(2, rank, wc), whole(2, rr, wc), whole(2, 8, 128), *[whole(rr, wc)] * 4,
            pl.BlockSpec(memory_space=pltpu.SMEM),
        ],
        out_specs=tuple(whole(rb, wc) for _ in range(4))
        + tuple(whole(rr, wc) for _ in range(4))
        + tuple(pl.BlockSpec((rb, wc), lambda j: (j, 0)) for _ in range(2)),
        compiler_params=pltpu.CompilerParams(vmem_limit_bytes=63 * 1024 * 1024),
        name="finish",
    )(wi, wg, all_w, ball, dirs, small, squares, fi, si, fg, sg, count)


def solution(mesh):
    cut, rows = P("fs", "tp"), P("fs", None)
    return jax.shard_map(
        functools.partial(shards, mesh.shape["fs"], mesh.shape["tp"]),
        mesh=mesh,
        in_specs=(rows, cut, cut, cut, cut, rows, rows, cut, cut, cut, cut),
        out_specs=(cut,) * 8 + (P(None, "tp"),) * 2,
        check_vma=False,
    )
```

```python
import functools

import jax
import jax.numpy as jnp
from jax import lax
from jax.experimental import pallas as pl
from jax.experimental.pallas import tpu as pltpu
from jax.sharding import PartitionSpec as P

first_decay = 0.8
second_decay = 0.95
learn_rate = 0.01
ANY = pl.BlockSpec(memory_space=pl.ANY)
VMEM = pl.BlockSpec(memory_space=pltpu.VMEM)
MESH = pl.DeviceIdType.MESH
f32, bf16 = jnp.float32, jnp.bfloat16


def moments(small, first, second):
    first_new = first_decay * first + (1.0 - first_decay) * small
    second_new = second_decay * second + (1.0 - second_decay) * small * small
    return first_new, second_new


def remote(src, dst, send, recv, **axis):
    return pltpu.make_async_remote_copy(
        src_ref=src, dst_ref=dst, send_sem=send, recv_sem=recv, device_id=axis, device_id_type=MESH
    )


def exchange(
    n, tp, x_hbm, ci_hbm, cg_hbm, wi_hbm, wg_hbm, bi_hbm, bg_hbm, fi, si, fg, sg,
    weights, basis_out, dir_out, small_out, squares_out,
    xs, cs, ball, wf, wb, proj, acc, part, recvp, dirs, dirf, sq,
    xsem, csem, bsem, wsem, osem,
    b_s, b_r, x_s, x_r, c_s, c_r, d_s, d_r, p_s, p_r, g_s, g_r, q_s, q_r,
    r_s, r_r, l_s, l_r, y_s, y_r,
):
    me, t = lax.axis_index("fs"), lax.axis_index("tp")
    tokens, rb, rank2 = xs.shape[1], ball.shape[1], ball.shape[2]
    group = xs.shape[2] // rb
    rank = rank2 // 2
    rr = rank // n
    wc = cs.shape[2]
    quarter = rb // 4
    tile = min(512, tokens)

    def local(src, dst, sem):
        copy = pltpu.make_async_copy(src, dst, sem)
        copy.start()
        return copy

    def peer(k):
        return lax.rem(me + k, n)

    def origin(k):
        return lax.rem(me + n - k, n)

    b_in = [
        local(ref, ball.at[me, :, pl.ds(p * rank, rank)], bsem.at[p])
        for p, ref in enumerate((bi_hbm, bg_hbm))
    ]
    x_in = []
    wide = rb * group
    for k in range(n // group):
        at = pl.multiple_of(origin(k) * rb, rb) if group == 1 else k * wide
        x_in.append(local(x_hbm.at[:, pl.ds(at, wide)], xs.at[k], xsem.at[k]))
    w_in = [local(ref, wf.at[p], wsem.at[p]) for p, ref in enumerate((wi_hbm, wg_hbm))]
    c_in = [local(ref, cs.at[p], csem.at[p]) for p, ref in enumerate((ci_hbm, cg_hbm))]

    barrier = pltpu.get_barrier_semaphore()
    for k in range(1, n):
        pl.semaphore_signal(barrier, inc=1, device_id={"fs": peer(k)}, device_id_type=MESH)
    for k in range(1, tp):
        pl.semaphore_signal(barrier, inc=1, device_id={"tp": lax.rem(t + k, tp)}, device_id_type=MESH)
    pl.semaphore_wait(barrier, n + tp - 2)

    q = lax.rem(t, 4)
    base = t - q
    qx = lax.rem(q + 2, 4)
    qc = q + 1 - 2 * lax.rem(q, 2)
    qd = lax.rem(qc + 2, 4)

    def rows(j, which):
        return ball.at[j, pl.ds(pl.multiple_of(which * quarter, quarter), quarter), :]

    for copy in b_in:
        copy.wait()
    pending = []
    b_copies = {}
    for k in range(1, n):
        b_copies[k] = remote(rows(me, q), rows(me, q), b_s.at[k], b_r.at[k], fs=peer(k))
        b_copies[k].start()
        pending.append(b_copies[k])

    def product(k, j):
        x_in[k].wait()

        def body(i, _):
            at = pl.ds(pl.multiple_of(i * tile, tile), tile)
            right = ball[j] if group == 1 else ball[j:j + group].reshape(wide, rank2)
            term = jnp.dot(xs[k, at, :], right, preferred_element_type=f32)
            if k == 0:
                proj[at, :] = term
            else:
                proj[at, :] += term
            return 0

        lax.fori_loop(0, tokens // tile, body, 0)

    def got(ref, sem):
        pltpu.make_async_copy(ref, ref, sem).wait()

    length = n // 2
    a, b = me // 2, lax.rem(me, 2)
    waits = []

    def block(chain, side, p):
        return weights.at[jnp.clip(chain, 0, length - 1) * 2 + side, p]

    def guarded(here, copy):
        @pl.when(here)
        def _():
            copy.start()

        waits.append((here, copy))

    def across(s, sign, p):
        chain = a - sign * (s - 1)
        exists = jnp.logical_and(chain >= 0, chain < length)
        place = block(chain, b, p)
        slot = ((s - 1) * 2 + (0 if sign == 1 else 1)) * 2 + p
        guarded(exists, remote(
            wb.at[p] if s == 1 else place, place, y_s.at[slot], y_r.at[slot], fs=a * 2 + 1 - b))

    def along(s, sign, p):
        chain = a - sign * (s - 1)
        exists = jnp.logical_and(chain >= 0, chain < length)
        place = block(chain, b, p)
        ss, sr = (r_s, r_r) if sign == 1 else (l_s, l_r)
        if s > 1:
            @pl.when(exists)
            def _():
                got(place, sr.at[(s - 1) * 2 + p])
        if s < length:
            after = a + sign
            inside = jnp.logical_and(after >= 0, after < length)
            to = jnp.clip(after, 0, length - 1) * 2 + b
            at = s * 2 + p
            guarded(jnp.logical_and(exists, inside), remote(
                wb.at[p] if s == 1 else place, place, ss.at[at], sr.at[at], fs=to))

    def send_weights(s):
        for p in range(2):
            for sign in (1, -1):
                along(s, sign, p)
                across(s, sign, p)

    for p in range(2):
        w_in[p].wait()
        wb[p] = wf[p].astype(bf16)

    for k in range(n + 2):
        if 1 <= k < n:
            j = origin(k)
            got(rows(j, q), b_r.at[k])
            for ss, sr, to in ((x_s, x_r, qx), (c_s, c_r, qc)):
                copy = remote(rows(j, q), rows(j, q), ss.at[k], sr.at[k], tp=base + to)
                copy.start()
                pending.append(copy)
        if 1 <= k - 1 < n:
            j = origin(k - 1)
            got(rows(j, qx), x_r.at[k - 1])
            copy = remote(rows(j, qx), rows(j, qx), d_s.at[k - 1], d_r.at[k - 1], tp=base + qc)
            copy.start()
            pending.append(copy)
        if k == 0:
            if group == 1:
                product(0, me)
            for p in range(2):
                across(1, 1, p)
        if k == 1:
            for p in range(2):
                for sign in (1, -1):
                    along(1, sign, p)
        if k >= 3:
            j = origin(k - 2)
            got(rows(j, qc), c_r.at[k - 2])
            got(rows(j, qd), d_r.at[k - 2])
            if group == 1:
                product(k - 2, j)
    if group > 1:
        for k in range(n // group):
            product(k, k * group)

    send_weights(2)

    for p in range(2):
        c_in[p].wait()

        def body(i, _):
            at = pl.ds(pl.multiple_of(i * tile, tile), tile)
            term = lax.dot_general(
                proj[at, p * rank:(p + 1) * rank].astype(bf16), cs[p, at, :],
                (((0,), (0,)), ((), ())), preferred_element_type=f32,
            )
            acc[p] += term
            return 0

        acc[p] = jnp.zeros_like(acc[p])
        lax.fori_loop(0, tokens // tile, body, 0)
        for j in range(n):
            part[j, p] = acc[p, j * rr:(j + 1) * rr, :].astype(bf16)
    for k in range(1, n):
        copy = remote(part.at[peer(k)], recvp.at[k], p_s.at[k], p_r.at[k], fs=peer(k))
        copy.start()
        pending.append(copy)
    out_basis = local(ball, basis_out, osem.at[0])
    own = pl.ds(pl.multiple_of(me * rr, rr), rr)
    total = acc[:, own, :]
    for k in range(1, n):
        got(recvp.at[k], p_r.at[k])
        total = total + recvp[k].astype(f32)
    small_out[...] = total
    for p, (first, second) in enumerate(((fi, si), (fg, sg))):
        first_new, second_new = moments(total[p], first[...], second[...])
        dirs[0, p] = (first_new / (jnp.sqrt(second_new) + 1e-08)).astype(bf16)
    for k in range(1, n):
        copy = remote(dirs.at[0], dirs.at[k], g_s.at[k], g_r.at[k], fs=peer(k))
        copy.start()
        pending.append(copy)
    for s in range(3, length + 1):
        if s == 3:
            send_weights(s)
    dirf[:, own, :] = dirs[0].astype(f32)
    for k in range(1, n):
        got(dirs.at[k], g_r.at[k])
        dirf[:, pl.ds(pl.multiple_of(origin(k) * rr, rr), rr), :] = dirs[k].astype(f32)
    for p in range(2):
        dir_out[p] = dirf[p].astype(bf16)
        sq[0, p] = jnp.zeros_like(sq[0, p])

        def body(j, _):
            update = jnp.dot(
                ball[j, :, p * rank:(p + 1) * rank], dir_out[p], preferred_element_type=f32
            )
            square = jnp.sum((update * update).reshape(rb // 8, 8, wc), axis=0)
            lanes = square[:, :128]
            for at in range(128, wc, 128):
                lanes = lanes + square[:, at:at + 128]
            sq[0, p] += lanes
            return 0

        lax.fori_loop(0, n, body, 0)
    for k in range(1, tp):
        copy = remote(sq.at[0], sq.at[k], q_s.at[k], q_r.at[k], tp=lax.rem(t + k, tp))
        copy.start()
        pending.append(copy)
    for s in range(4, length + 1):
        send_weights(s)
    summed = sq[0]
    for k in range(1, tp):
        got(sq.at[k], q_r.at[k])
        summed = summed + sq[k]
    squares_out[...] = summed
    out_basis.wait()
    for s in range(1, length + 1):
        for sign in (1, -1):
            if s == 1 and sign == -1:
                continue
            chain = a - sign * (s - 1)
            slot = ((s - 1) * 2 + (0 if sign == 1 else 1)) * 2
            for p in range(2):

                @pl.when(jnp.logical_and(chain >= 0, chain < length))
                def _():
                    got(block(chain, 1 - b, p), y_r.at[slot + p])
    for here, copy in waits:
        @pl.when(here)
        def _():
            copy.wait_send()
    for copy in pending:
        copy.wait_send()


def finish(
    wi, wg, all_w, ball, dirs, small, squares, fi, si, fg, sg, count_ref,
    new_i, new_g, step_i, step_g, fi_new, si_new, fg_new, sg_new, copy_i, copy_g,
):
    j = pl.program_id(0)
    me = lax.axis_index("fs")
    rank = dirs.shape[1]

    @pl.when(j == 0)
    def _():
        fi_new[...], si_new[...] = moments(small[0], fi[...], si[...])
        fg_new[...], sg_new[...] = moments(small[1], fg[...], sg[...])

    for p, (w, new, step, copy) in enumerate(((wi, new_i, step_i, copy_i), (wg, new_g, step_g, copy_g))):
        mean = jnp.sum(squares[p], keepdims=True) * count_ref[0]
        factor = jnp.minimum(1.0, 1.0 / jnp.sqrt(mean + 1e-06))
        update = jnp.dot(ball[0, :, p * rank:(p + 1) * rank], dirs[p], preferred_element_type=f32)
        scaled = factor * update

        @pl.when(j == me)
        def _():
            step[...] = scaled
            fresh = w[...] - learn_rate * scaled
            new[...] = fresh
            copy[...] = fresh.astype(bf16)

        @pl.when(j != me)
        def _():
            copy[...] = (all_w[0, p].astype(f32) - learn_rate * scaled).astype(bf16)


def shards(n, tp, x, ci, cg, wi, wg, bi, bg, fi, si, fg, sg):
    tokens, width = x.shape
    wc, (rb, rank), rr = ci.shape[1], bi.shape, fi.shape[0]
    length = n // 2
    group = max(1, 128 // rb)
    dma = pltpu.SemaphoreType.DMA
    all_w, ball, dirs, small, squares = pl.pallas_call(
        functools.partial(exchange, n, tp),
        out_shape=(
            jax.ShapeDtypeStruct((n, 2, rb, wc), bf16),
            jax.ShapeDtypeStruct((n, rb, 2 * rank), bf16),
            jax.ShapeDtypeStruct((2, rank, wc), bf16),
            jax.ShapeDtypeStruct((2, rr, wc), f32),
            jax.ShapeDtypeStruct((2, 8, 128), f32),
        ),
        in_specs=[ANY] * 7 + [VMEM] * 4,
        out_specs=(ANY, ANY, VMEM, VMEM, VMEM),
        scratch_shapes=[
            pltpu.VMEM((n // group, tokens, rb * group), bf16),
            pltpu.VMEM((2, tokens, wc), bf16),
            pltpu.VMEM((n, rb, 2 * rank), bf16),
            pltpu.VMEM((2, rb, wc), f32),
            pltpu.VMEM((2, rb, wc), bf16),
            pltpu.VMEM((tokens, 2 * rank), f32),
            pltpu.VMEM((2, rank, wc), f32),
            pltpu.VMEM((n, 2, rr, wc), bf16),
            pltpu.VMEM((n, 2, rr, wc), bf16),
            pltpu.VMEM((n, 2, rr, wc), bf16),
            pltpu.VMEM((2, rank, wc), f32),
            pltpu.VMEM((tp, 2, 8, 128), f32),
            dma((n,)), dma((2,)), dma((2,)), dma((2,)), dma((1,)),
        ]
        + [dma((n,))] * 12
        + [dma((tp,))] * 2
        + [dma((2 * length,))] * 4
        + [dma((4 * length,))] * 2,
        compiler_params=pltpu.CompilerParams(
            collective_id=0, has_side_effects=True, vmem_limit_bytes=56 * 1024 * 1024
        ),
        name="exchange",
    )(x, ci, cg, wi, wg, bi, bg, fi, si, fg, sg)

    def whole(*shape):
        return pl.BlockSpec(shape, lambda j: (0,) * len(shape))

    count = jnp.full((1,), 1.0 / (width * wc * tp), f32)
    return pl.pallas_call(
        finish,
        grid=(n,),
        out_shape=tuple(jax.ShapeDtypeStruct((rb, wc), f32) for _ in range(4))
        + tuple(jax.ShapeDtypeStruct((rr, wc), f32) for _ in range(4))
        + tuple(jax.ShapeDtypeStruct((width, wc), bf16) for _ in range(2)),
        in_specs=[
            whole(rb, wc), whole(rb, wc),
            pl.BlockSpec((1, 2, rb, wc), lambda j: (j, 0, 0, 0)),
            pl.BlockSpec((1, rb, 2 * rank), lambda j: (j, 0, 0)),
            whole(2, rank, wc), whole(2, rr, wc), whole(2, 8, 128), *[whole(rr, wc)] * 4,
            pl.BlockSpec(memory_space=pltpu.SMEM),
        ],
        out_specs=tuple(whole(rb, wc) for _ in range(4))
        + tuple(whole(rr, wc) for _ in range(4))
        + tuple(pl.BlockSpec((rb, wc), lambda j: (j, 0)) for _ in range(2)),
        compiler_params=pltpu.CompilerParams(vmem_limit_bytes=63 * 1024 * 1024),
        name="finish",
    )(wi, wg, all_w, ball, dirs, small, squares, fi, si, fg, sg, count)


def solution(mesh):
    cut, rows = P("fs", "tp"), P("fs", None)
    return jax.shard_map(
        functools.partial(shards, mesh.shape["fs"], mesh.shape["tp"]),
        mesh=mesh,
        in_specs=(rows, cut, cut, cut, cut, rows, rows, cut, cut, cut, cut),
        out_specs=(cut,) * 8 + (P(None, "tp"),) * 2,
        check_vma=False,
    )
```
